32 devices in a mesh: grp: 2 (over x), tp: 4 (over z), dp: 4 (over y, core).
Axes of the slice: x: 2, y: 2, z: 4, core: 2. Of those that a mesh axis runs over, the one named last changes fastest.
Arguments:
- stream: bfloat16 [32, 4096], P('grp', 'dp'), parts along dimension 0, may hold values from -11 to 11
- states: float32 [2, 32, 32, 64, 64], P(None, ('grp', 'dp'), 'tp'), parts along dimension 1, may hold values from -6 to 6
- norm_gain: bfloat16 [2, 4096], P(None, 'dp'), may hold values from 0.099609375 to 1.8984375
- recept_weight: bfloat16 [2, 4096, 2048], P(None, 'dp', 'tp'), may hold values from -0.09375 to 0.09375
- key_weight: bfloat16 [2, 4096, 2048], P(None, 'dp', 'tp'), may hold values from -0.09375 to 0.09375
- value_weight: bfloat16 [2, 4096, 2048], P(None, 'dp', 'tp'), may hold values from -0.09375 to 0.09375
- decay_weight: bfloat16 [2, 4096, 2048], P(None, 'dp', 'tp'), may hold values from -0.09375 to 0.09375
- rate_weight: bfloat16 [2, 4096, 2048], P(None, 'dp', 'tp'), may hold values from -0.09375 to 0.09375
- gate_weight: bfloat16 [2, 4096, 2048], P(None, 'dp', 'tp'), may hold values from -0.09375 to 0.09375
- out_weight: bfloat16 [2, 2048, 4096], P(None, 'tp', 'dp'), may hold values from -0.125 to 0.125
- decay_bias: float32 [2, 2048], P(None, 'tp'), may hold values from -2 to 2
- head_gain: bfloat16 [2, 2048], P(None, 'tp'), may hold values from 0.099609375 to 1.8984375
Outputs:
- new_stream: bfloat16 [32, 4096], P('grp', 'dp'), parts along dimension 0
- new_states: float32 [2, 32, 32, 64, 64], P(None, ('grp', 'dp'), 'tp'), parts along dimension 1
The draws below stay inside these ranges and needn't reach their ends.
There are 2 independent parts, one for each index of `grp`. The reference program is written for one: setup_inputs(seed, part) draws one part's arguments, and reference() takes and returns one part's arrays. A program takes and returns all parts, laid end to end along the dimension named above; an argument that names none is the same for every part. Nothing has to cross between parts.
All inputs are finite; a program needn't handle non-finite values.
Results may differ from the reference program's by a relative error of at most 0.0068.
Values may be sent and summed in bfloat16 or wider, within the bound.
No kernel may reach another device: no remote copies, remote signals or barrier semaphores. Data moves between devices by JAX's collectives and lax.ppermute only.
A program may use at most 64 MiB of HBM per device.

```python
import jax
import jax.numpy as jnp
from jax import lax

D = 4096
INNER = 2048
HEAD = 64
HEADS = 32
SEQS = 16


def draw_stream(key, part):
    first, second = jax.random.split(jax.random.fold_in(key, 11), 2)
    columns = jnp.arange(D, dtype=jnp.float32) / D
    rough = jax.random.uniform(second, (D,), jnp.float32, 0.5, 1.5)
    scales = 0.6 * jnp.power(3.0, columns) * rough
    base = jnp.clip(jax.random.normal(first, (SEQS, D), jnp.float32), -4.0, 4.0)
    values = base * scales[None, :]
    return jnp.clip(values, -11.0, 11.0).astype(jnp.bfloat16)


def levels(stream_key, shape, cuts, smallest, high):
    def one(axis_at, blocks):
        draws = jax.random.uniform(jax.random.fold_in(jax.random.fold_in(stream_key, 6), axis_at), (blocks,), jnp.float32, smallest / len(cuts), high / len(cuts))
        return jnp.repeat(jnp.exp(draws), shape[axis_at] // blocks).reshape((-1,) + (1,) * (len(shape) - axis_at - 1))

    level = one(*cuts[0])
    for cut in cuts[1:]:
        level = level * one(*cut)
    return level


def gaussian(rng, dims, deviation, bound, cuts=(), held_as=jnp.bfloat16):
    values = deviation * jax.random.normal(rng, dims, jnp.float32)
    if cuts:
        values = values * levels(rng, dims, cuts, -0.22, 0.18)
    return jnp.clip(values, -bound, bound).astype(held_as)


def setup_inputs(seed: int = 0, part: int = 0) -> dict:
    key_of = jax.random.split(jax.random.key(seed), 13)
    own_keys = jax.random.split(jax.random.fold_in(key_of[12], part), 13)
    stream = draw_stream(jax.random.fold_in(jax.random.fold_in(key_of[12], part), 71), part)
    states = gaussian(own_keys[1], (2, SEQS, HEADS, HEAD, HEAD), 0.5, 6.0, ((1, 4), (2, 4)), jnp.float32)
    norm_gain = jnp.clip(1.0 + 0.18 * jax.random.normal(key_of[2], (2, D), jnp.float32), 0.099609375, 1.8984375).astype(jnp.bfloat16)
    recept_weight = gaussian(key_of[3], (2, D, INNER), D ** -0.5, 0.09375, ((1, 4), (2, 4)))
    key_weight = gaussian(key_of[4], (2, D, INNER), D ** -0.5, 0.09375, ((1, 4), (2, 4)))
    value_weight = gaussian(key_of[5], (2, D, INNER), D ** -0.5, 0.09375, ((1, 4), (2, 4)))
    decay_weight = gaussian(key_of[6], (2, D, INNER), D ** -0.5, 0.09375, ((1, 4), (2, 4)))
    rate_weight = gaussian(key_of[7], (2, D, INNER), D ** -0.5, 0.09375, ((1, 4), (2, 4)))
    gate_weight = gaussian(key_of[8], (2, D, INNER), D ** -0.5, 0.09375, ((1, 4), (2, 4)))
    out_weight = gaussian(key_of[9], (2, INNER, D), INNER ** -0.5, 0.125, ((1, 4), (2, 4)))
    decay_bias = jnp.clip(jax.random.uniform(key_of[10], (2, INNER), jnp.float32, -2.0, 2.0) * levels(key_of[10], (2, INNER), ((1, 4),), -0.4, 0.0), -2.0, 2.0)
    head_gain = jnp.clip(1.0 + 0.18 * jax.random.normal(key_of[11], (2, INNER), jnp.float32), 0.099609375, 1.8984375).astype(jnp.bfloat16)
    return {"stream": stream, "states": states, "norm_gain": norm_gain, "recept_weight": recept_weight, "key_weight": key_weight, "value_weight": value_weight, "decay_weight": decay_weight, "rate_weight": rate_weight, "gate_weight": gate_weight, "out_weight": out_weight, "decay_bias": decay_bias, "head_gain": head_gain}


def run_block(stream, state_blk, gain, weights, out_weight, bias, hgain):
    current = stream.astype(jnp.float32)
    inv_rms = lax.rsqrt(lax.optimization_barrier(jnp.mean(current * current, axis=1, keepdims=True)) + 1e-06)
    normed = (current * gain.astype(jnp.float32)).astype(jnp.bfloat16)
    seqs = stream.shape[0]
    projected = [(jnp.dot(normed, weight, preferred_element_type=jnp.float32) * inv_rms).reshape(seqs, -1, HEAD) for weight in weights]
    recept, key_vec, value_vec, decay_pre, rate_pre, gate_pre = projected
    unit_key = key_vec * lax.rsqrt(lax.optimization_barrier(jnp.sum(key_vec * key_vec, axis=2, keepdims=True)) + 1e-06)
    rate_vec = jax.nn.sigmoid(rate_pre)
    decay = jnp.exp(-0.606531 * jax.nn.sigmoid(bias.reshape(1, -1, HEAD) + decay_pre))
    removed = jnp.einsum('bhij,bhj->bhi', state_blk, unit_key, precision=lax.Precision.HIGHEST)
    new_state = state_blk * decay[:, :, None, :] - removed[..., None] * (unit_key * rate_vec)[:, :, None, :] + value_vec[..., None] * key_vec[:, :, None, :]
    read = jnp.einsum('bhij,bhj->bhi', new_state, recept, precision=lax.Precision.HIGHEST)
    center = read - lax.optimization_barrier(jnp.mean(read, axis=2, keepdims=True))
    normal_read = center * lax.rsqrt(lax.optimization_barrier(jnp.mean(center * center, axis=2, keepdims=True)) + 1e-05)
    gated = normal_read * hgain.astype(jnp.float32).reshape(1, -1, HEAD) * jax.nn.sigmoid(gate_pre)
    mixed = gated.reshape(seqs, -1).astype(jnp.bfloat16)
    branch = jnp.dot(mixed, out_weight, preferred_element_type=jnp.float32)
    return ((current + branch).astype(jnp.bfloat16), new_state)

def reference(stream, states, norm_gain, recept_weight, key_weight, value_weight, decay_weight, rate_weight, gate_weight, out_weight, decay_bias, head_gain):
    current = stream
    fresh_list = []
    for layer in range(2):
        weights = (recept_weight[layer], key_weight[layer], value_weight[layer], decay_weight[layer], rate_weight[layer], gate_weight[layer])
        current, fresh = run_block(current, states[layer], norm_gain[layer], weights, out_weight[layer], decay_bias[layer], head_gain[layer])
        fresh_list.append(fresh)
    return (current, jnp.stack(fresh_list))
```

```python
import jax
import jax.numpy as jnp
from jax import lax
from jax.sharding import PartitionSpec as P

HEAD = 64
RS = "pp"
AG = "pp"
BR = "pp"


def axis_len(name):
    return lax.psum(1, name)


def exchange_sum(part, axis):
    n = axis_len(axis)
    rows = part.shape[0] // n
    if RS == "a2a":
        sent = part.astype(jnp.bfloat16).reshape(n, rows, -1)
        got = lax.all_to_all(sent, axis, 0, 0)
        return jnp.sum(got.astype(jnp.float32), axis=0)
    me = lax.axis_index(axis)
    blocks = part.astype(jnp.bfloat16).reshape(n, rows, -1)
    total = lax.dynamic_index_in_dim(blocks, me, 0, keepdims=False).astype(jnp.float32)
    got = []
    for step in range(1, n):
        block = lax.dynamic_index_in_dim(blocks, (me + step) % n, 0, keepdims=False)
        got.append(lax.ppermute(block, axis, [(i, (i + step) % n) for i in range(n)]))
    for g in got:
        total = total + g.astype(jnp.float32)
    return total


def gather_rows(x, axis):
    n = axis_len(axis)
    if AG == "ag":
        return lax.all_gather(x, axis, axis=0, tiled=True)
    me = lax.axis_index(axis)
    pieces = [x] + [
        lax.ppermute(x, axis, [(i, (i + s) % n) for i in range(n)]) for s in range(1, n)
    ]
    stack = jnp.stack(pieces)
    order = (me - jnp.arange(n)) % n
    return jnp.take(stack, order, axis=0).reshape(n * x.shape[0], -1)


def sum_over(part, axis):
    n = axis_len(axis)
    sent = part.astype(jnp.bfloat16)
    if BR == "ag":
        got = lax.all_gather(sent, axis, axis=0)
        return jnp.sum(got.astype(jnp.float32), axis=0)
    got = [lax.ppermute(sent, axis, [(i, (i + s) % n) for i in range(n)]) for s in range(1, n)]
    total = sent.astype(jnp.float32)
    for g in got:
        total = total + g.astype(jnp.float32)
    return total


def run_block(stream, state_blk, gain, weights, out_weight, bias, hgain):
    width = weights[0].shape[1]
    features = stream.shape[1] * axis_len("dp")
    local_rows = state_blk.shape[0]
    current = stream.astype(jnp.float32)
    squares = jnp.sum(current * current, axis=1, keepdims=True)
    high = squares.astype(jnp.bfloat16).astype(jnp.float32)
    low = squares - high
    normed = (current * gain.astype(jnp.float32)).astype(jnp.bfloat16)
    lane = lax.broadcasted_iota(jnp.int32, (stream.shape[0], 128), 1)
    extra = jnp.where(lane == 0, high, jnp.where(lane == 1, low, 0.0))
    parts = [jnp.dot(normed, w, preferred_element_type=jnp.float32) for w in weights]
    summed = exchange_sum(jnp.concatenate(parts + [extra], axis=1), "dp")
    totals = summed[:, 6 * width] + summed[:, 6 * width + 1]
    inv_rms = lax.rsqrt(totals / features + 1e-06)[:, None]
    projected = (summed[:, : 6 * width] * inv_rms).reshape(local_rows, 6, -1, HEAD)
    recept = projected[:, 0]
    key_vec = projected[:, 1]
    value_vec = projected[:, 2]
    decay_pre = projected[:, 3]
    rate_pre = projected[:, 4]
    gate_pre = projected[:, 5]
    unit_key = key_vec * lax.rsqrt(jnp.sum(key_vec * key_vec, axis=2, keepdims=True) + 1e-06)
    rate_vec = jax.nn.sigmoid(rate_pre)
    decay = jnp.exp(-0.606531 * jax.nn.sigmoid(bias.reshape(1, -1, HEAD) + decay_pre))
    removed = jnp.sum(state_blk * unit_key[:, :, None, :], axis=3)
    new_state = (
        state_blk * decay[:, :, None, :]
        - removed[..., None] * (unit_key * rate_vec)[:, :, None, :]
        + value_vec[..., None] * key_vec[:, :, None, :]
    )
    read = jnp.sum(new_state * recept[:, :, None, :], axis=3)
    center = read - jnp.mean(read, axis=2, keepdims=True)
    normal_read = center * lax.rsqrt(jnp.mean(center * center, axis=2, keepdims=True) + 1e-05)
    gated = normal_read * hgain.astype(jnp.float32).reshape(1, -1, HEAD) * jax.nn.sigmoid(gate_pre)
    mixed = gated.reshape(local_rows, width).astype(jnp.bfloat16)
    branch_part = jnp.dot(gather_rows(mixed, "dp"), out_weight, preferred_element_type=jnp.float32)
    return ((current + sum_over(branch_part, "tp")).astype(jnp.bfloat16), new_state)


def per_device(
    stream,
    states,
    norm_gain,
    recept_weight,
    key_weight,
    value_weight,
    decay_weight,
    rate_weight,
    gate_weight,
    out_weight,
    decay_bias,
    head_gain,
):
    current = stream
    fresh_list = []
    for layer in range(2):
        weights = (
            recept_weight[layer],
            key_weight[layer],
            value_weight[layer],
            decay_weight[layer],
            rate_weight[layer],
            gate_weight[layer],
        )
        current, fresh = run_block(
            current,
            states[layer],
            norm_gain[layer],
            weights,
            out_weight[layer],
            decay_bias[layer],
            head_gain[layer],
        )
        fresh_list.append(fresh)
    return (current, jnp.stack(fresh_list))


def solution(mesh):
    in_specs = (
        P("grp", "dp"),
        P(None, ("grp", "dp"), "tp", None, None),
        P(None, "dp"),
        P(None, "dp", "tp"),
        P(None, "dp", "tp"),
        P(None, "dp", "tp"),
        P(None, "dp", "tp"),
        P(None, "dp", "tp"),
        P(None, "dp", "tp"),
        P(None, "tp", "dp"),
        P(None, "tp"),
        P(None, "tp"),
    )
    out_specs = (P("grp", "dp"), P(None, ("grp", "dp"), "tp", None, None))
    return jax.shard_map(
        per_device, mesh=mesh, in_specs=in_specs, out_specs=out_specs, check_vma=False
    )
```

```python
import functools

import jax
import jax.numpy as jnp
from jax import lax
from jax.experimental import pallas as pl
from jax.experimental.pallas import tpu as pltpu
from jax.sharding import PartitionSpec as P

ROLES = 6
EXTRA = 128

VMEM = pl.BlockSpec(memory_space=pltpu.VMEM)
SMEM = pl.BlockSpec(memory_space=pltpu.SMEM)
HBM = pl.BlockSpec(memory_space=pl.ANY)
CHUNKS = 2


def f32(x):
    return x.astype(jnp.float32)


def project_kernel(layer, n, fused, me_ref, stream_ref, gain_ref, *refs):
    branch_refs, refs = refs[:fused], refs[fused:]
    weight_refs, refs = refs[:ROLES], refs[ROLES:]
    own_ref, sent_refs, refs = refs[0], refs[1:n], refs[n:]
    if fused:
        current_ref, refs = refs[0], refs[1:]
    buf, sems = refs
    depth, width = buf.shape[1:]
    step = depth // CHUNKS
    copies = []
    for r in range(ROLES):
        for c in range(CHUNKS):
            rows = pl.ds(c * step, step)
            copy = pltpu.make_async_copy(
                weight_refs[r].at[layer, rows], buf.at[r, rows], sems.at[r, c]
            )
            copy.start()
            copies.append(copy)
    current = f32(stream_ref[...])
    if fused:
        total = branch_refs[0][...]
        for ref in branch_refs[1:]:
            total = total + f32(ref[...])
        rounded = (current + total).astype(jnp.bfloat16)
        current_ref[...] = rounded
        current = f32(rounded)
    seqs = current.shape[0]
    rows = seqs // n
    current = pltpu.roll(current, (n - me_ref[0]) * rows % seqs, 0)
    squares = jnp.sum(current * current, axis=1, keepdims=True)
    high = f32(squares.astype(jnp.bfloat16))
    lane = lax.broadcasted_iota(jnp.int32, (seqs, EXTRA), 1)
    extra = jnp.where(lane == 0, high, jnp.where(lane == 1, squares - high, 0.0))
    normed = (current * f32(gain_ref[layer : layer + 1, :])).astype(jnp.bfloat16)

    def emit(part, start, size):
        own_ref[:, start : start + size] = part[:rows]
        for s in range(1, n):
            sent_refs[s - 1][:, start : start + size] = part[s * rows : (s + 1) * rows].astype(
                jnp.bfloat16
            )

    emit(extra, ROLES * width, EXTRA)
    for r in range(ROLES):
        for c in range(CHUNKS):
            copies[r * CHUNKS + c].wait()
        emit(jnp.dot(normed, buf[r], preferred_element_type=jnp.float32), r * width, width)


def project(layer, me, stream, branches, gain, weights, n):
    seqs = stream.shape[0]
    depth, width = weights[0].shape[1:]
    rows = seqs // n
    cols = ROLES * width + EXTRA
    outs = [jax.ShapeDtypeStruct((rows, cols), jnp.float32)]
    outs += [jax.ShapeDtypeStruct((rows, cols), jnp.bfloat16)] * (n - 1)
    if branches:
        outs.append(jax.ShapeDtypeStruct(stream.shape, jnp.bfloat16))
    got = pl.pallas_call(
        functools.partial(project_kernel, layer, n, len(branches)),
        in_specs=[SMEM, VMEM, VMEM] + [VMEM] * len(branches) + [HBM] * ROLES,
        out_specs=[VMEM] * len(outs),
        out_shape=outs,
        scratch_shapes=[
            pltpu.VMEM((ROLES, depth, width), jnp.bfloat16),
            pltpu.SemaphoreType.DMA((ROLES, CHUNKS)),
        ],
        compiler_params=pltpu.CompilerParams(vmem_limit_bytes=16 << 20),
        name=f"project{layer}",
    )(me, stream, gain, *branches, *weights)
    current = got[n] if branches else stream
    return got[:n], current


def mix_kernel(layer, features, n, own_ref, *refs):
    got_refs, refs = refs[: n - 1], refs[n - 1 :]
    bias_ref, hgain_ref, states_ref, mixed_ref, vec_ref, buf, read_buf, sems = refs
    seqs, heads, head = buf.shape[:3]
    width = heads * head
    copies = []
    for q in range(seqs):
        copy = pltpu.make_async_copy(states_ref.at[layer, q], buf.at[q], sems.at[q])
        copy.start()
        copies.append(copy)
    total = own_ref[...]
    for ref in got_refs:
        total = total + f32(ref[...])
    squares = total[:, ROLES * width : ROLES * width + 1]
    squares = squares + total[:, ROLES * width + 1 : ROLES * width + 2]
    total = total * lax.rsqrt(squares / features + 1e-06)

    def by_head(x):
        return jnp.concatenate([x[:, h * head : (h + 1) * head] for h in range(heads)], axis=0)

    def spread(ref):
        return by_head(jnp.broadcast_to(f32(ref[layer : layer + 1, :]), (seqs, width)))

    recept, key, value, decay_pre, rate_pre, gate_pre = [
        by_head(total[:, r * width : (r + 1) * width]) for r in range(ROLES)
    ]
    unit = key * lax.rsqrt(jnp.sum(key * key, axis=1, keepdims=True) + 1e-06)
    unit_rate = unit * jax.nn.sigmoid(rate_pre)
    decay = jnp.exp(-0.606531 * jax.nn.sigmoid(spread(bias_ref) + decay_pre))
    for i, vec in enumerate((unit, unit_rate, decay, value, key)):
        vec_ref[i] = vec
    weight = decay * recept - jnp.sum(unit_rate * recept, axis=1, keepdims=True) * unit
    along = jnp.sum(key * recept, axis=1, keepdims=True) * value
    eye = lax.broadcasted_iota(jnp.int32, (head, head), 0) == lax.broadcasted_iota(
        jnp.int32, (head, head), 1
    )
    for q in range(seqs):
        copies[q].wait()
        for h in range(heads):
            b = h * seqs + q
            column = jnp.sum(buf[q, h] * weight[b : b + 1], axis=1, keepdims=True)
            read_buf[b : b + 1, :] = jnp.sum(
                jnp.where(eye, column, 0.0), axis=0, keepdims=True
            )
    read = read_buf[...] + along
    center = read - jnp.mean(read, axis=1, keepdims=True)
    normal = center * lax.rsqrt(jnp.mean(center * center, axis=1, keepdims=True) + 1e-05)
    gated = normal * spread(hgain_ref) * jax.nn.sigmoid(gate_pre)
    for h in range(heads):
        mixed_ref[:, h * head : (h + 1) * head] = gated[h * seqs : (h + 1) * seqs].astype(
            jnp.bfloat16
        )


def mix(layer, features, own, got, bias, hgain, states):
    seqs, heads, head = states.shape[1:4]
    return pl.pallas_call(
        functools.partial(mix_kernel, layer, features, len(got) + 1),
        in_specs=[VMEM] * (len(got) + 3) + [HBM],
        out_specs=[VMEM, VMEM],
        out_shape=[
            jax.ShapeDtypeStruct((seqs, heads * head), jnp.bfloat16),
            jax.ShapeDtypeStruct((5, seqs * heads, head), jnp.float32),
        ],
        scratch_shapes=[
            pltpu.VMEM((seqs, heads, head, head), jnp.float32),
            pltpu.VMEM((seqs * heads, head), jnp.float32),
            pltpu.SemaphoreType.DMA((seqs,)),
        ],
        compiler_params=pltpu.CompilerParams(vmem_limit_bytes=16 << 20),
        name=f"mix{layer}",
    )(own, *got, bias, hgain, states)


def update_kernel(layer, vec_ref, states_ref, *refs):
    out_ref, buf, fresh, sems, out_sems = refs[-5:]
    seqs, heads, head = buf.shape[:3]
    copies = []
    for q in range(seqs):
        copy = pltpu.make_async_copy(states_ref.at[layer, q], buf.at[q], sems.at[q])
        copy.start()
        copies.append(copy)
    eye = lax.broadcasted_iota(jnp.int32, (head, head), 0) == lax.broadcasted_iota(
        jnp.int32, (head, head), 1
    )
    unit, unit_rate, decay, value, key = [vec_ref[i] for i in range(5)]
    writes = []
    for q in range(seqs):
        copies[q].wait()
        for h in range(heads):
            b = h * seqs + q
            state = buf[q, h]
            removed = jnp.sum(state * unit[b : b + 1], axis=1, keepdims=True)
            column = jnp.sum(jnp.where(eye, value[b : b + 1], 0.0), axis=1, keepdims=True)
            fresh[q, h] = (
                state * decay[b : b + 1]
                - removed * unit_rate[b : b + 1]
                + column * key[b : b + 1]
            )
        write = pltpu.make_async_copy(fresh.at[q], out_ref.at[layer, q], out_sems.at[q])
        write.start()
        writes.append(write)
    for write in writes:
        write.wait()


def update(layer, vecs, states, previous):
    block = states.shape[1:]
    extra = [] if previous is None else [previous]
    return pl.pallas_call(
        functools.partial(update_kernel, layer),
        in_specs=[VMEM, HBM] + [HBM] * len(extra),
        out_specs=HBM,
        out_shape=jax.ShapeDtypeStruct(states.shape, states.dtype),
        input_output_aliases={2: 0} if extra else {},
        scratch_shapes=[
            pltpu.VMEM(block, jnp.float32),
            pltpu.VMEM(block, jnp.float32),
            pltpu.SemaphoreType.DMA((block[0],)),
            pltpu.SemaphoreType.DMA((block[0],)),
        ],
        compiler_params=pltpu.CompilerParams(vmem_limit_bytes=16 << 20),
        cost_estimate=pl.CostEstimate(flops=10**6, bytes_accessed=4 << 20, transcendentals=0),
        name=f"update{layer}",
    )(vecs, states, *extra)


def out_kernel(layer, me_ref, *refs):
    weight_ref, own_ref, sent_ref = refs[-3:]
    parts = refs[:-3]
    rows = parts[0].shape[0]
    mixed = jnp.concatenate([f32(ref[...]) for ref in parts], axis=0).astype(jnp.bfloat16)
    part = jnp.dot(mixed, weight_ref[layer], preferred_element_type=jnp.float32)
    part = pltpu.roll(part, me_ref[0] * rows, 0)
    own_ref[...] = part
    sent_ref[...] = part.astype(jnp.bfloat16)


def out_project(layer, me, parts, weight):
    shape = (len(parts) * parts[0].shape[0], weight.shape[2])
    return pl.pallas_call(
        functools.partial(out_kernel, layer),
        in_specs=[SMEM] + [VMEM] * (len(parts) + 1),
        out_specs=[VMEM, VMEM],
        out_shape=[
            jax.ShapeDtypeStruct(shape, jnp.float32),
            jax.ShapeDtypeStruct(shape, jnp.bfloat16),
        ],
        compiler_params=pltpu.CompilerParams(vmem_limit_bytes=16 << 20),
        name=f"out{layer}",
    )(me, *parts, weight)


def shift(x, axis, n, s):
    return lax.ppermute(x, axis, [(i, (i + s) % n) for i in range(n)])


def per_device(n_dp, n_tp, stream, states, norm_gain, *rest):
    weights = rest[:ROLES]
    out_weight, decay_bias, head_gain = rest[ROLES:]
    me = lax.axis_index("dp").astype(jnp.int32).reshape(1)
    features = stream.shape[1] * n_dp
    current = stream
    branches = []
    fresh = None
    for layer in range(states.shape[0]):
        (own, *sent), current = project(layer, me, current, branches, norm_gain, weights, n_dp)
        got = [shift(x, "dp", n_dp, s + 1) for s, x in enumerate(sent)]
        mixed, vecs = mix(layer, features, own, got, decay_bias, head_gain, states)
        pieces = [mixed] + [shift(mixed, "dp", n_dp, n_dp - t) for t in range(1, n_dp)]
        fresh = update(layer, vecs, states, fresh)
        part, part_sent = out_project(layer, me, pieces, out_weight)
        branches = [part] + [shift(part_sent, "tp", n_tp, s) for s in range(1, n_tp)]
    total = branches[0]
    for x in branches[1:]:
        total = total + f32(x)
    return (f32(current) + total).astype(jnp.bfloat16), fresh


def solution(mesh):
    in_specs = (
        P("grp", "dp"),
        P(None, ("grp", "dp"), "tp", None, None),
        P(None, "dp"),
        P(None, "dp", "tp"),
        P(None, "dp", "tp"),
        P(None, "dp", "tp"),
        P(None, "dp", "tp"),
        P(None, "dp", "tp"),
        P(None, "dp", "tp"),
        P(None, "tp", "dp"),
        P(None, "tp"),
        P(None, "tp"),
    )
    out_specs = (P("grp", "dp"), P(None, ("grp", "dp"), "tp", None, None))
    return jax.shard_map(
        functools.partial(per_device, mesh.shape["dp"], mesh.shape["tp"]),
        mesh=mesh,
        in_specs=in_specs,
        out_specs=out_specs,
        check_vma=False,
    )
```

```python
import functools

import jax
import jax.numpy as jnp
from jax import lax
from jax.experimental import pallas as pl
from jax.experimental.pallas import tpu as pltpu
from jax.sharding import PartitionSpec as P

ROLES = 6
EXTRA = 128

VMEM = pl.BlockSpec(memory_space=pltpu.VMEM)
SMEM = pl.BlockSpec(memory_space=pltpu.SMEM)
HBM = pl.BlockSpec(memory_space=pltpu.HBM)
CHUNKS = 2


def f32(x):
    return x.astype(jnp.float32)


def emit_projections(n, me, current, gain, weight_of, own_ref, sent_refs):
    seqs = current.shape[0]
    rows = seqs // n
    current = pltpu.roll(current, (n - me) * rows % seqs, 0)
    squares = jnp.sum(current * current, axis=1, keepdims=True)
    high = f32(squares.astype(jnp.bfloat16))
    lane = lax.broadcasted_iota(jnp.int32, (seqs, EXTRA), 1)
    extra = jnp.where(lane == 0, high, jnp.where(lane == 1, squares - high, 0.0))
    normed = (current * gain).astype(jnp.bfloat16)
    width = (own_ref.shape[1] - EXTRA) // ROLES

    def emit(part, start, size):
        own_ref[:, start : start + size] = part[:rows]
        for s in range(1, n):
            sent_refs[s - 1][:, start : start + size] = part[s * rows : (s + 1) * rows].astype(
                jnp.bfloat16
            )

    emit(extra, ROLES * width, EXTRA)
    for r in range(ROLES):
        weight = weight_of(r)
        emit(jnp.dot(normed, weight, preferred_element_type=jnp.float32), r * width, width)


def first_kernel(n, me_ref, stream_ref, gain_ref, *refs):
    weight_refs, refs = refs[:ROLES], refs[ROLES:]
    own_ref, sent_refs, refs = refs[0], refs[1:n], refs[n:]
    stream_buf, gain_buf, buf, small_sems, sems = refs
    small = [
        pltpu.make_async_copy(stream_ref, stream_buf, small_sems.at[0]),
        pltpu.make_async_copy(gain_ref, gain_buf, small_sems.at[1]),
    ]
    for copy in small:
        copy.start()
    step = buf.shape[1] // CHUNKS
    copies = []
    for r in range(ROLES):
        for c in range(CHUNKS):
            rows = pl.ds(c * step, step)
            copy = pltpu.make_async_copy(
                weight_refs[r].at[0, rows], buf.at[r, rows], sems.at[r, c]
            )
            copy.start()
            copies.append(copy)
    for copy in small:
        copy.wait()

    def weight_of(r):
        for c in range(CHUNKS):
            copies[r * CHUNKS + c].wait()
        return buf[r]

    emit_projections(
        n, me_ref[0], f32(stream_buf[...]), f32(gain_buf[0:1, :]), weight_of, own_ref, sent_refs
    )


def next_kernel(layer, n, fused, me_ref, stream_ref, gain_ref, *refs):
    branch_refs, refs = refs[:fused], refs[fused:]
    weight_refs, refs = refs[:ROLES], refs[ROLES + 1 :]
    own_ref, sent_refs, current_ref = refs[0], refs[1:n], refs[n]
    total = branch_refs[0][...]
    for ref in branch_refs[1:]:
        total = total + f32(ref[...])
    rounded = (f32(stream_ref[...]) + total).astype(jnp.bfloat16)
    current_ref[...] = rounded
    emit_projections(
        n,
        me_ref[0],
        f32(rounded),
        f32(gain_ref[layer : layer + 1, :]),
        lambda r: weight_refs[r][layer],
        own_ref,
        sent_refs,
    )


def project(layer, me, stream, branches, gain, weights, n, fresh):
    seqs = stream.shape[0]
    depth, width = weights[0].shape[1:]
    rows = seqs // n
    cols = ROLES * width + EXTRA
    outs = [jax.ShapeDtypeStruct((rows, cols), jnp.float32)]
    outs += [jax.ShapeDtypeStruct((rows, cols), jnp.bfloat16)] * (n - 1)
    if not layer:
        stream_in, gain, *weights = [
            pltpu.with_memory_space_constraint(x, pltpu.HBM) for x in (stream, gain, *weights)
        ]
        got = pl.pallas_call(
            functools.partial(first_kernel, n),
            in_specs=[SMEM] + [HBM] * (ROLES + 2),
            out_specs=[VMEM] * len(outs),
            out_shape=outs,
            scratch_shapes=[
                pltpu.VMEM(stream.shape, stream.dtype),
                pltpu.VMEM(gain.shape, gain.dtype),
                pltpu.VMEM((ROLES, depth, width), jnp.bfloat16),
                pltpu.SemaphoreType.DMA((2,)),
                pltpu.SemaphoreType.DMA((ROLES, CHUNKS)),
            ],
            compiler_params=pltpu.CompilerParams(vmem_limit_bytes=12 << 20),
            name="project0",
        )(me, stream_in, gain, *weights)
        return got, stream
    outs.append(jax.ShapeDtypeStruct(stream.shape, jnp.bfloat16))
    got = pl.pallas_call(
        functools.partial(next_kernel, layer, n, len(branches)),
        in_specs=[SMEM, VMEM, VMEM] + [VMEM] * (len(branches) + ROLES) + [HBM],
        out_specs=[VMEM] * len(outs),
        out_shape=outs,
        compiler_params=pltpu.CompilerParams(vmem_limit_bytes=32 << 20),
        name=f"project{layer}",
    )(me, stream, gain, *branches, *weights, fresh)
    return got[:n], got[n]


def mix_kernel(layer, features, n, own_ref, *refs):
    got_refs, refs = refs[: n - 1], refs[n - 1 :]
    bias_ref, hgain_ref, states_ref, mixed_ref, vec_ref, read_buf = refs
    seqs, heads, head = states_ref.shape[1:4]
    width = heads * head
    total = own_ref[...]
    for ref in got_refs:
        total = total + f32(ref[...])
    squares = total[:, ROLES * width : ROLES * width + 1]
    squares = squares + total[:, ROLES * width + 1 : ROLES * width + 2]
    total = total * lax.rsqrt(squares / features + 1e-06)

    def by_head(x):
        return jnp.concatenate([x[:, h * head : (h + 1) * head] for h in range(heads)], axis=0)

    def spread(ref):
        return by_head(jnp.broadcast_to(f32(ref[layer : layer + 1, :]), (seqs, width)))

    recept, key, value, decay_pre, rate_pre, gate_pre = [
        by_head(total[:, r * width : (r + 1) * width]) for r in range(ROLES)
    ]
    unit = key * lax.rsqrt(jnp.sum(key * key, axis=1, keepdims=True) + 1e-06)
    unit_rate = unit * jax.nn.sigmoid(rate_pre)
    decay = jnp.exp(-0.606531 * jax.nn.sigmoid(spread(bias_ref) + decay_pre))
    for i, vec in enumerate((unit, unit_rate, decay, value, key)):
        vec_ref[i] = vec
    weight = decay * recept - jnp.sum(unit_rate * recept, axis=1, keepdims=True) * unit
    along = jnp.sum(key * recept, axis=1, keepdims=True) * value
    eye = lax.broadcasted_iota(jnp.int32, (head, head), 0) == lax.broadcasted_iota(
        jnp.int32, (head, head), 1
    )
    for q in range(seqs):
        for h in range(heads):
            b = h * seqs + q
            column = jnp.sum(states_ref[layer, q, h] * weight[b : b + 1], axis=1, keepdims=True)
            read_buf[b : b + 1, :] = jnp.sum(
                jnp.where(eye, column, 0.0), axis=0, keepdims=True
            )
    read = read_buf[...] + along
    center = read - jnp.mean(read, axis=1, keepdims=True)
    normal = center * lax.rsqrt(jnp.mean(center * center, axis=1, keepdims=True) + 1e-05)
    gated = normal * spread(hgain_ref) * jax.nn.sigmoid(gate_pre)
    for h in range(heads):
        mixed_ref[:, h * head : (h + 1) * head] = gated[h * seqs : (h + 1) * seqs].astype(
            jnp.bfloat16
        )


def mix(layer, features, own, got, bias, hgain, states):
    seqs, heads, head = states.shape[1:4]
    return pl.pallas_call(
        functools.partial(mix_kernel, layer, features, len(got) + 1),
        in_specs=[VMEM] * (len(got) + 4),
        out_specs=[VMEM, VMEM],
        out_shape=[
            jax.ShapeDtypeStruct((seqs, heads * head), jnp.bfloat16),
            jax.ShapeDtypeStruct((5, seqs * heads, head), jnp.float32),
        ],
        scratch_shapes=[
            pltpu.VMEM((seqs * heads, head), jnp.float32),
        ],
        compiler_params=pltpu.CompilerParams(vmem_limit_bytes=16 << 20),
        name=f"mix{layer}",
    )(own, *got, bias, hgain, states)


def update_kernel(layer, vec_ref, states_ref, *refs):
    out_ref, buf, fresh, sems, out_sems = refs[-5:]
    seqs, heads, head = buf.shape[:3]
    copies = []
    for q in range(seqs):
        copy = pltpu.make_async_copy(states_ref.at[layer, q], buf.at[q], sems.at[q])
        copy.start()
        copies.append(copy)
    eye = lax.broadcasted_iota(jnp.int32, (head, head), 0) == lax.broadcasted_iota(
        jnp.int32, (head, head), 1
    )
    unit, unit_rate, decay, value, key = [vec_ref[i] for i in range(5)]
    writes = []
    for q in range(seqs):
        copies[q].wait()
        for h in range(heads):
            b = h * seqs + q
            state = buf[q, h]
            removed = jnp.sum(state * unit[b : b + 1], axis=1, keepdims=True)
            column = jnp.sum(jnp.where(eye, value[b : b + 1], 0.0), axis=1, keepdims=True)
            fresh[q, h] = (
                state * decay[b : b + 1]
                - removed * unit_rate[b : b + 1]
                + column * key[b : b + 1]
            )
        write = pltpu.make_async_copy(fresh.at[q], out_ref.at[layer, q], out_sems.at[q])
        write.start()
        writes.append(write)
    for write in writes:
        write.wait()


def update(layer, vecs, states, previous):
    block = states.shape[1:]
    extra = [] if previous is None else [previous]
    return pl.pallas_call(
        functools.partial(update_kernel, layer),
        in_specs=[VMEM, HBM] + [HBM] * len(extra),
        out_specs=HBM,
        out_shape=jax.ShapeDtypeStruct(states.shape, states.dtype),
        input_output_aliases={2: 0} if extra else {},
        scratch_shapes=[
            pltpu.VMEM(block, jnp.float32),
            pltpu.VMEM(block, jnp.float32),
            pltpu.SemaphoreType.DMA((block[0],)),
            pltpu.SemaphoreType.DMA((block[0],)),
        ],
        compiler_params=pltpu.CompilerParams(vmem_limit_bytes=16 << 20),
        cost_estimate=pl.CostEstimate(flops=10**6, bytes_accessed=4 << 20, transcendentals=0),
        name=f"update{layer}",
    )(vecs, states, *extra)


def out_kernel(layer, me_ref, *refs):
    weight_ref, own_ref, sent_ref = refs[-3:]
    parts = refs[:-3]
    rows = parts[0].shape[0]
    mixed = jnp.concatenate([f32(ref[...]) for ref in parts], axis=0).astype(jnp.bfloat16)
    part = jnp.dot(mixed, weight_ref[layer], preferred_element_type=jnp.float32)
    part = pltpu.roll(part, me_ref[0] * rows, 0)
    own_ref[...] = part
    sent_ref[...] = part.astype(jnp.bfloat16)


def out_project(layer, me, parts, weight):
    shape = (len(parts) * parts[0].shape[0], weight.shape[2])
    return pl.pallas_call(
        functools.partial(out_kernel, layer),
        in_specs=[SMEM] + [VMEM] * (len(parts) + 1),
        out_specs=[VMEM, VMEM],
        out_shape=[
            jax.ShapeDtypeStruct(shape, jnp.float32),
            jax.ShapeDtypeStruct(shape, jnp.bfloat16),
        ],
        compiler_params=pltpu.CompilerParams(vmem_limit_bytes=16 << 20),
        name=f"out{layer}",
    )(me, *parts, weight)


def shift(x, axis, n, s):
    return lax.ppermute(x, axis, [(i, (i + s) % n) for i in range(n)])


def per_device(n_dp, n_tp, stream, states, norm_gain, *rest):
    weights = rest[:ROLES]
    out_weight, decay_bias, head_gain = rest[ROLES:]
    me = lax.axis_index("dp").astype(jnp.int32).reshape(1)
    features = stream.shape[1] * n_dp
    current = stream
    branches = []
    fresh = None
    for layer in range(states.shape[0]):
        (own, *sent), current = project(
            layer, me, current, branches, norm_gain, weights, n_dp, fresh
        )
        got = [shift(x, "dp", n_dp, s + 1) for s, x in enumerate(sent)]
        mixed, vecs = mix(layer, features, own, got, decay_bias, head_gain, states)
        pieces = [mixed] + [shift(mixed, "dp", n_dp, n_dp - t) for t in range(1, n_dp)]
        fresh = update(layer, vecs, states, fresh)
        part, part_sent = out_project(layer, me, pieces, out_weight)
        branches = [part] + [shift(part_sent, "tp", n_tp, s) for s in range(1, n_tp)]
    total = branches[0]
    for x in branches[1:]:
        total = total + f32(x)
    return (f32(current) + total).astype(jnp.bfloat16), fresh


def solution(mesh):
    in_specs = (
        P("grp", "dp"),
        P(None, ("grp", "dp"), "tp", None, None),
        P(None, "dp"),
        P(None, "dp", "tp"),
        P(None, "dp", "tp"),
        P(None, "dp", "tp"),
        P(None, "dp", "tp"),
        P(None, "dp", "tp"),
        P(None, "dp", "tp"),
        P(None, "tp", "dp"),
        P(None, "tp"),
        P(None, "tp"),
    )
    out_specs = (P("grp", "dp"), P(None, ("grp", "dp"), "tp", None, None))
    return jax.shard_map(
        functools.partial(per_device, mesh.shape["dp"], mesh.shape["tp"]),
        mesh=mesh,
        in_specs=in_specs,
        out_specs=out_specs,
        check_vma=False,
    )
```

```python
import functools

import jax
import jax.numpy as jnp
from jax import lax
from jax.experimental import pallas as pl
from jax.experimental.pallas import tpu as pltpu
from jax.sharding import PartitionSpec as P

ROLES = 6
EXTRA = 128

VMEM = pl.BlockSpec(memory_space=pltpu.VMEM)
SMEM = pl.BlockSpec(memory_space=pltpu.SMEM)
HBM = pl.BlockSpec(memory_space=pltpu.HBM)
CHUNKS = 2


def f32(x):
    return x.astype(jnp.float32)


def swap_blocks(x, me, rows, n):
    seqs = x.shape[0]
    row = lax.broadcasted_iota(jnp.int32, x.shape, 0)
    for k in range(n.bit_length() - 1):
        step = rows << k
        upper = row < 0
        for start in range(step, seqs, 2 * step):
            upper = upper | ((row >= start) & (row < start + step))
        swapped = pltpu.roll(x, step, 0)
        if 2 * step < seqs:
            swapped = jnp.where(upper, swapped, pltpu.roll(x, seqs - step, 0))
        x = jnp.where(lax.broadcast((me >> k) & 1, x.shape) == 1, swapped, x)
    return x


def emit_projections(n, me, current, gain, weight_of, own_ref, sent_refs):
    seqs = current.shape[0]
    rows = seqs // n
    current = swap_blocks(current, me, rows, n)
    squares = jnp.sum(current * current, axis=1, keepdims=True)
    high = f32(squares.astype(jnp.bfloat16))
    lane = lax.broadcasted_iota(jnp.int32, (seqs, EXTRA), 1)
    extra = jnp.where(lane == 0, high, jnp.where(lane == 1, squares - high, 0.0))
    normed = (current * gain).astype(jnp.bfloat16)
    width = (own_ref.shape[1] - EXTRA) // ROLES

    def emit(part, start, size):
        own_ref[:, start : start + size] = part[:rows]
        for s in range(1, n):
            sent_refs[s - 1][:, start : start + size] = part[s * rows : (s + 1) * rows].astype(
                jnp.bfloat16
            )

    emit(extra, ROLES * width, EXTRA)
    for r in range(ROLES):
        weight = weight_of(r)
        emit(jnp.dot(normed, weight, preferred_element_type=jnp.float32), r * width, width)


def first_kernel(n, me_ref, stream_ref, gain_ref, *refs):
    weight_refs, refs = refs[:ROLES], refs[ROLES:]
    own_ref, sent_refs, refs = refs[0], refs[1:n], refs[n:]
    stream_buf, gain_buf, buf, small_sems, sems = refs
    small = [
        pltpu.make_async_copy(stream_ref, stream_buf, small_sems.at[0]),
        pltpu.make_async_copy(gain_ref, gain_buf, small_sems.at[1]),
    ]
    for copy in small:
        copy.start()
    step = buf.shape[1] // CHUNKS
    copies = []
    for r in range(ROLES):
        for c in range(CHUNKS):
            rows = pl.ds(c * step, step)
            copy = pltpu.make_async_copy(
                weight_refs[r].at[0, rows], buf.at[r, rows], sems.at[r, c]
            )
            copy.start()
            copies.append(copy)
    for copy in small:
        copy.wait()

    def weight_of(r):
        for c in range(CHUNKS):
            copies[r * CHUNKS + c].wait()
        return buf[r]

    emit_projections(
        n, me_ref[0], f32(stream_buf[...]), f32(gain_buf[0:1, :]), weight_of, own_ref, sent_refs
    )


def next_kernel(layer, n, fused, me_ref, stream_ref, gain_ref, *refs):
    branch_refs, refs = refs[:fused], refs[fused:]
    weight_refs, refs = refs[:ROLES], refs[ROLES + 1 :]
    own_ref, sent_refs, current_ref = refs[0], refs[1:n], refs[n]
    total = branch_refs[0][...]
    for ref in branch_refs[1:]:
        total = total + f32(ref[...])
    rounded = (f32(stream_ref[...]) + total).astype(jnp.bfloat16)
    current_ref[...] = rounded
    emit_projections(
        n,
        me_ref[0],
        f32(rounded),
        f32(gain_ref[layer : layer + 1, :]),
        lambda r: weight_refs[r][layer],
        own_ref,
        sent_refs,
    )


def project(layer, me, stream, branches, gain, weights, n, fresh):
    seqs = stream.shape[0]
    depth, width = weights[0].shape[1:]
    rows = seqs // n
    cols = ROLES * width + EXTRA
    outs = [jax.ShapeDtypeStruct((rows, cols), jnp.float32)]
    outs += [jax.ShapeDtypeStruct((rows, cols), jnp.bfloat16)] * (n - 1)
    if not layer:
        stream_in, gain, *weights = [
            pltpu.with_memory_space_constraint(x, pltpu.HBM) for x in (stream, gain, *weights)
        ]
        got = pl.pallas_call(
            functools.partial(first_kernel, n),
            in_specs=[SMEM] + [HBM] * (ROLES + 2),
            out_specs=[VMEM] * len(outs),
            out_shape=outs,
            scratch_shapes=[
                pltpu.VMEM(stream.shape, stream.dtype),
                pltpu.VMEM(gain.shape, gain.dtype),
                pltpu.VMEM((ROLES, depth, width), jnp.bfloat16),
                pltpu.SemaphoreType.DMA((2,)),
                pltpu.SemaphoreType.DMA((ROLES, CHUNKS)),
            ],
            compiler_params=pltpu.CompilerParams(vmem_limit_bytes=12 << 20),
            name="project0",
        )(me, stream_in, gain, *weights)
        return got, stream
    outs.append(jax.ShapeDtypeStruct(stream.shape, jnp.bfloat16))
    got = pl.pallas_call(
        functools.partial(next_kernel, layer, n, len(branches)),
        in_specs=[SMEM, VMEM, VMEM] + [VMEM] * (len(branches) + ROLES) + [HBM],
        out_specs=[VMEM] * len(outs),
        out_shape=outs,
        compiler_params=pltpu.CompilerParams(vmem_limit_bytes=32 << 20),
        name=f"project{layer}",
    )(
        me,
        stream,
        gain,
        *branches,
        *weights,
        pltpu.with_memory_space_constraint(fresh, pltpu.HBM),
    )
    return got[:n], got[n]


def mix_kernel(layer, features, n, own_ref, *refs):
    got_refs, refs = refs[: n - 1], refs[n - 1 :]
    bias_ref, hgain_ref, states_ref, mixed_ref, vec_ref, read_buf = refs
    seqs, heads, head = states_ref.shape[1:4]
    width = heads * head
    total = own_ref[...]
    for ref in got_refs:
        total = total + f32(ref[...])
    squares = total[:, ROLES * width : ROLES * width + 1]
    squares = squares + total[:, ROLES * width + 1 : ROLES * width + 2]
    total = total * lax.rsqrt(squares / features + 1e-06)

    def by_head(x):
        return jnp.concatenate([x[:, h * head : (h + 1) * head] for h in range(heads)], axis=0)

    def spread(ref):
        return by_head(jnp.broadcast_to(f32(ref[layer : layer + 1, :]), (seqs, width)))

    recept, key, value, decay_pre, rate_pre, gate_pre = [
        by_head(total[:, r * width : (r + 1) * width]) for r in range(ROLES)
    ]
    unit = key * lax.rsqrt(jnp.sum(key * key, axis=1, keepdims=True) + 1e-06)
    unit_rate = unit * jax.nn.sigmoid(rate_pre)
    decay = jnp.exp(-0.606531 * jax.nn.sigmoid(spread(bias_ref) + decay_pre))
    for i, vec in enumerate((unit, unit_rate, decay, value, key)):
        vec_ref[i] = vec
    weight = decay * recept - jnp.sum(unit_rate * recept, axis=1, keepdims=True) * unit
    along = jnp.sum(key * recept, axis=1, keepdims=True) * value
    eye = lax.broadcasted_iota(jnp.int32, (head, head), 0) == lax.broadcasted_iota(
        jnp.int32, (head, head), 1
    )
    for q in range(seqs):
        for h in range(heads):
            b = h * seqs + q
            column = jnp.sum(states_ref[layer, q, h] * weight[b : b + 1], axis=1, keepdims=True)
            read_buf[b : b + 1, :] = jnp.sum(
                jnp.where(eye, column, 0.0), axis=0, keepdims=True
            )
    read = read_buf[...] + along
    center = read - jnp.mean(read, axis=1, keepdims=True)
    normal = center * lax.rsqrt(jnp.mean(center * center, axis=1, keepdims=True) + 1e-05)
    gated = normal * spread(hgain_ref) * jax.nn.sigmoid(gate_pre)
    for h in range(heads):
        mixed_ref[:, h * head : (h + 1) * head] = gated[h * seqs : (h + 1) * seqs].astype(
            jnp.bfloat16
        )


def mix(layer, features, own, got, bias, hgain, states):
    seqs, heads, head = states.shape[1:4]
    return pl.pallas_call(
        functools.partial(mix_kernel, layer, features, len(got) + 1),
        in_specs=[VMEM] * (len(got) + 4),
        out_specs=[VMEM, VMEM],
        out_shape=[
            jax.ShapeDtypeStruct((seqs, heads * head), jnp.bfloat16),
            jax.ShapeDtypeStruct((5, seqs * heads, head), jnp.float32),
        ],
        scratch_shapes=[
            pltpu.VMEM((seqs * heads, head), jnp.float32),
        ],
        compiler_params=pltpu.CompilerParams(vmem_limit_bytes=16 << 20),
        name=f"mix{layer}",
    )(own, *got, bias, hgain, states)


def update_kernel(layer, vec_ref, states_ref, *refs):
    out_ref, buf, fresh, sems, out_sems = refs[-5:]
    seqs, heads, head = buf.shape[:3]
    copies = []
    for q in range(seqs):
        copy = pltpu.make_async_copy(states_ref.at[layer, q], buf.at[q], sems.at[q])
        copy.start()
        copies.append(copy)
    eye = lax.broadcasted_iota(jnp.int32, (head, head), 0) == lax.broadcasted_iota(
        jnp.int32, (head, head), 1
    )
    unit, unit_rate, decay, value, key = [vec_ref[i] for i in range(5)]
    writes = []
    for q in range(seqs):
        copies[q].wait()
        for h in range(heads):
            b = h * seqs + q
            state = buf[q, h]
            removed = jnp.sum(state * unit[b : b + 1], axis=1, keepdims=True)
            column = jnp.sum(jnp.where(eye, value[b : b + 1], 0.0), axis=1, keepdims=True)
            fresh[q, h] = (
                state * decay[b : b + 1]
                - removed * unit_rate[b : b + 1]
                + column * key[b : b + 1]
            )
        write = pltpu.make_async_copy(fresh.at[q], out_ref.at[layer, q], out_sems.at[q])
        write.start()
        writes.append(write)
    for write in writes:
        write.wait()


def update(layer, vecs, states, previous):
    block = states.shape[1:]
    extra = [] if previous is None else [previous]
    return pl.pallas_call(
        functools.partial(update_kernel, layer),
        in_specs=[VMEM, HBM] + [HBM] * len(extra),
        out_specs=HBM,
        out_shape=jax.ShapeDtypeStruct(states.shape, states.dtype),
        input_output_aliases={2: 0} if extra else {},
        scratch_shapes=[
            pltpu.VMEM(block, jnp.float32),
            pltpu.VMEM(block, jnp.float32),
            pltpu.SemaphoreType.DMA((block[0],)),
            pltpu.SemaphoreType.DMA((block[0],)),
        ],
        compiler_params=pltpu.CompilerParams(vmem_limit_bytes=16 << 20),
        cost_estimate=pl.CostEstimate(flops=10**6, bytes_accessed=4 << 20, transcendentals=0),
        name=f"update{layer}",
    )(vecs, states, *extra)


def out_kernel(layer, me_ref, *refs):
    weight_ref, own_ref, sent_ref = refs[-3:]
    parts = refs[:-3]
    rows = parts[0].shape[0]
    mixed = jnp.concatenate([f32(ref[...]) for ref in parts], axis=0).astype(jnp.bfloat16)
    part = jnp.dot(mixed, weight_ref[layer], preferred_element_type=jnp.float32)
    part = swap_blocks(part, me_ref[0], rows, len(parts))
    own_ref[...] = part
    sent_ref[...] = part.astype(jnp.bfloat16)


def out_project(layer, me, parts, weight):
    shape = (len(parts) * parts[0].shape[0], weight.shape[2])
    return pl.pallas_call(
        functools.partial(out_kernel, layer),
        in_specs=[SMEM] + [VMEM] * (len(parts) + 1),
        out_specs=[VMEM, VMEM],
        out_shape=[
            jax.ShapeDtypeStruct(shape, jnp.float32),
            jax.ShapeDtypeStruct(shape, jnp.bfloat16),
        ],
        compiler_params=pltpu.CompilerParams(vmem_limit_bytes=16 << 20),
        name=f"out{layer}",
    )(me, *parts, weight)


def swap(x, axis, n, s):
    return lax.ppermute(x, axis, [(i, i ^ s) for i in range(n)])


def send_order(n, near_first):
    steps = list(range(1, n))
    return steps if near_first else steps[::-1]


def per_device(n_dp, n_tp, stream, states, norm_gain, *rest):
    weights = rest[:ROLES]
    out_weight, decay_bias, head_gain = rest[ROLES:]
    me = lax.axis_index("dp").astype(jnp.int32).reshape(1)
    features = stream.shape[1] * n_dp
    current = stream
    branches = []
    fresh = None
    for layer in range(states.shape[0]):
        (own, *sent), current = project(
            layer, me, current, branches, norm_gain, weights, n_dp, fresh
        )
        got = [swap(sent[s - 1], "dp", n_dp, s) for s in send_order(n_dp, True)]
        mixed, vecs = mix(layer, features, own, got, decay_bias, head_gain, states)
        pieces = {s: swap(mixed, "dp", n_dp, s) for s in send_order(n_dp, True)}
        pieces = [mixed] + [pieces[s] for s in range(1, n_dp)]
        fresh = update(layer, vecs, states, fresh)
        part, part_sent = out_project(layer, me, pieces, out_weight)
        branches = [part] + [swap(part_sent, "tp", n_tp, s) for s in send_order(n_tp, True)]
    total = branches[0]
    for x in branches[1:]:
        total = total + f32(x)
    return (f32(current) + total).astype(jnp.bfloat16), fresh


def solution(mesh):
    in_specs = (
        P("grp", "dp"),
        P(None, ("grp", "dp"), "tp", None, None),
        P(None, "dp"),
        P(None, "dp", "tp"),
        P(None, "dp", "tp"),
        P(None, "dp", "tp"),
        P(None, "dp", "tp"),
        P(None, "dp", "tp"),
        P(None, "dp", "tp"),
        P(None, "tp", "dp"),
        P(None, "tp"),
        P(None, "tp"),
    )
    out_specs = (P("grp", "dp"), P(None, ("grp", "dp"), "tp", None, None))
    return jax.shard_map(
        functools.partial(per_device, mesh.shape["dp"], mesh.shape["tp"]),
        mesh=mesh,
        in_specs=in_specs,
        out_specs=out_specs,
        check_vma=False,
    )
```

```python
import functools

import jax
import jax.numpy as jnp
from jax import lax
from jax.experimental import pallas as pl
from jax.experimental.pallas import tpu as pltpu
from jax.sharding import PartitionSpec as P

ROLES = 6
EXTRA = 128

VMEM = pl.BlockSpec(memory_space=pltpu.VMEM)
SMEM = pl.BlockSpec(memory_space=pltpu.SMEM)
HBM = pl.BlockSpec(memory_space=pltpu.HBM)
CHUNKS = 1


def f32(x):
    return x.astype(jnp.float32)


def swap_blocks(x, me, rows, n):
    seqs = x.shape[0]
    row = lax.broadcasted_iota(jnp.int32, x.shape, 0)
    for k in range(n.bit_length() - 1):
        step = rows << k
        upper = row < 0
        for start in range(step, seqs, 2 * step):
            upper = upper | ((row >= start) & (row < start + step))
        swapped = pltpu.roll(x, step, 0)
        if 2 * step < seqs:
            swapped = jnp.where(upper, swapped, pltpu.roll(x, seqs - step, 0))
        x = jnp.where(lax.broadcast((me >> k) & 1, x.shape) == 1, swapped, x)
    return x


def emit_projections(n, me, current, gain, weight_of, own_ref, sent_refs):
    seqs = current.shape[0]
    rows = seqs // n
    current = swap_blocks(current, me, rows, n)
    squares = jnp.sum(current * current, axis=1, keepdims=True)
    high = f32(squares.astype(jnp.bfloat16))
    lane = lax.broadcasted_iota(jnp.int32, (seqs, EXTRA), 1)
    extra = jnp.where(lane == 0, high, jnp.where(lane == 1, squares - high, 0.0))
    normed = (current * gain).astype(jnp.bfloat16)
    width = (own_ref.shape[1] - EXTRA) // ROLES

    def emit(part, start, size):
        own_ref[:, start : start + size] = part[:rows]
        for s in range(1, n):
            sent_refs[s - 1][:, start : start + size] = part[s * rows : (s + 1) * rows].astype(
                jnp.bfloat16
            )

    emit(extra, ROLES * width, EXTRA)
    for r in range(ROLES):
        weight = weight_of(r)
        emit(jnp.dot(normed, weight, preferred_element_type=jnp.float32), r * width, width)


def first_kernel(n, me_ref, stream_ref, gain_ref, *refs):
    weight_refs, refs = refs[:ROLES], refs[ROLES:]
    own_ref, sent_refs, refs = refs[0], refs[1:n], refs[n:]
    stream_buf, gain_buf, buf, small_sems, sems = refs
    small = [
        pltpu.make_async_copy(stream_ref, stream_buf, small_sems.at[0]),
        pltpu.make_async_copy(gain_ref, gain_buf, small_sems.at[1]),
    ]
    for copy in small:
        copy.start()
    step = buf.shape[1] // CHUNKS
    copies = []
    for r in range(ROLES):
        for c in range(CHUNKS):
            rows = pl.ds(c * step, step)
            copy = pltpu.make_async_copy(
                weight_refs[r].at[0, rows], buf.at[r, rows], sems.at[r, c]
            )
            copy.start()
            copies.append(copy)
    for copy in small:
        copy.wait()

    def weight_of(r):
        for c in range(CHUNKS):
            copies[r * CHUNKS + c].wait()
        return buf[r]

    emit_projections(
        n, me_ref[0], f32(stream_buf[...]), f32(gain_buf[0:1, :]), weight_of, own_ref, sent_refs
    )


def next_kernel(layer, n, fused, me_ref, stream_ref, gain_ref, *refs):
    branch_refs, refs = refs[:fused], refs[fused:]
    weight_refs, refs = refs[:ROLES], refs[ROLES + 1 :]
    own_ref, sent_refs, current_ref = refs[0], refs[1:n], refs[n]
    total = branch_refs[0][...]
    for ref in branch_refs[1:]:
        total = total + f32(ref[...])
    rounded = (f32(stream_ref[...]) + total).astype(jnp.bfloat16)
    current_ref[...] = rounded
    emit_projections(
        n,
        me_ref[0],
        f32(rounded),
        f32(gain_ref[layer : layer + 1, :]),
        lambda r: weight_refs[r][layer],
        own_ref,
        sent_refs,
    )


def project(layer, me, stream, branches, gain, weights, n, fresh):
    seqs = stream.shape[0]
    depth, width = weights[0].shape[1:]
    rows = seqs // n
    cols = ROLES * width + EXTRA
    outs = [jax.ShapeDtypeStruct((rows, cols), jnp.float32)]
    outs += [jax.ShapeDtypeStruct((rows, cols), jnp.bfloat16)] * (n - 1)
    if not layer:
        stream_in, gain, *weights = [
            pltpu.with_memory_space_constraint(x, pltpu.HBM) for x in (stream, gain, *weights)
        ]
        got = pl.pallas_call(
            functools.partial(first_kernel, n),
            in_specs=[SMEM] + [HBM] * (ROLES + 2),
            out_specs=[VMEM] * len(outs),
            out_shape=outs,
            scratch_shapes=[
                pltpu.VMEM(stream.shape, stream.dtype),
                pltpu.VMEM(gain.shape, gain.dtype),
                pltpu.VMEM((ROLES, depth, width), jnp.bfloat16),
                pltpu.SemaphoreType.DMA((2,)),
                pltpu.SemaphoreType.DMA((ROLES, CHUNKS)),
            ],
            compiler_params=pltpu.CompilerParams(vmem_limit_bytes=12 << 20),
            name="project0",
        )(me, stream_in, gain, *weights)
        return got, stream
    outs.append(jax.ShapeDtypeStruct(stream.shape, jnp.bfloat16))
    got = pl.pallas_call(
        functools.partial(next_kernel, layer, n, len(branches)),
        in_specs=[SMEM, VMEM, VMEM] + [VMEM] * (len(branches) + ROLES) + [HBM],
        out_specs=[VMEM] * len(outs),
        out_shape=outs,
        compiler_params=pltpu.CompilerParams(vmem_limit_bytes=32 << 20),
        name=f"project{layer}",
    )(
        me,
        stream,
        gain,
        *branches,
        *weights,
        pltpu.with_memory_space_constraint(fresh, pltpu.HBM),
    )
    return got[:n], got[n]


def mix_kernel(layer, features, n, own_ref, *refs):
    got_refs, refs = refs[: n - 1], refs[n - 1 :]
    bias_ref, hgain_ref, states_ref, mixed_ref, vec_ref, read_buf = refs
    seqs, heads, head = states_ref.shape[1:4]
    width = heads * head
    total = own_ref[...]
    for ref in got_refs:
        total = total + f32(ref[...])
    squares = total[:, ROLES * width : ROLES * width + 1]
    squares = squares + total[:, ROLES * width + 1 : ROLES * width + 2]
    total = total * lax.rsqrt(squares / features + 1e-06)

    def by_head(x):
        return jnp.concatenate([x[:, h * head : (h + 1) * head] for h in range(heads)], axis=0)

    def spread(ref):
        return by_head(jnp.broadcast_to(f32(ref[layer : layer + 1, :]), (seqs, width)))

    recept, key, value, decay_pre, rate_pre, gate_pre = [
        by_head(total[:, r * width : (r + 1) * width]) for r in range(ROLES)
    ]
    unit = key * lax.rsqrt(jnp.sum(key * key, axis=1, keepdims=True) + 1e-06)
    unit_rate = unit * jax.nn.sigmoid(rate_pre)
    decay = jnp.exp(-0.606531 * jax.nn.sigmoid(spread(bias_ref) + decay_pre))
    for i, vec in enumerate((unit, unit_rate, decay, value, key)):
        vec_ref[i] = vec
    weight = decay * recept - jnp.sum(unit_rate * recept, axis=1, keepdims=True) * unit
    along = jnp.sum(key * recept, axis=1, keepdims=True) * value
    eye = lax.broadcasted_iota(jnp.int32, (head, head), 0) == lax.broadcasted_iota(
        jnp.int32, (head, head), 1
    )
    for q in range(seqs):
        for h in range(heads):
            b = h * seqs + q
            column = jnp.sum(states_ref[layer, q, h] * weight[b : b + 1], axis=1, keepdims=True)
            read_buf[b : b + 1, :] = jnp.sum(
                jnp.where(eye, column, 0.0), axis=0, keepdims=True
            )
    read = read_buf[...] + along
    center = read - jnp.mean(read, axis=1, keepdims=True)
    normal = center * lax.rsqrt(jnp.mean(center * center, axis=1, keepdims=True) + 1e-05)
    gated = normal * spread(hgain_ref) * jax.nn.sigmoid(gate_pre)
    for h in range(heads):
        mixed_ref[:, h * head : (h + 1) * head] = gated[h * seqs : (h + 1) * seqs].astype(
            jnp.bfloat16
        )


def mix(layer, features, own, got, bias, hgain, states):
    seqs, heads, head = states.shape[1:4]
    return pl.pallas_call(
        functools.partial(mix_kernel, layer, features, len(got) + 1),
        in_specs=[VMEM] * (len(got) + 4),
        out_specs=[VMEM, VMEM],
        out_shape=[
            jax.ShapeDtypeStruct((seqs, heads * head), jnp.bfloat16),
            jax.ShapeDtypeStruct((5, seqs * heads, head), jnp.float32),
        ],
        scratch_shapes=[
            pltpu.VMEM((seqs * heads, head), jnp.float32),
        ],
        compiler_params=pltpu.CompilerParams(vmem_limit_bytes=16 << 20),
        name=f"mix{layer}",
    )(own, *got, bias, hgain, states)


def update_kernel(layer, vec_ref, states_ref, *refs):
    out_ref, buf, fresh, sems, out_sems = refs[-5:]
    seqs, heads, head = buf.shape[:3]
    copies = []
    for q in range(seqs):
        copy = pltpu.make_async_copy(states_ref.at[layer, q], buf.at[q], sems.at[q])
        copy.start()
        copies.append(copy)
    eye = lax.broadcasted_iota(jnp.int32, (head, head), 0) == lax.broadcasted_iota(
        jnp.int32, (head, head), 1
    )
    unit, unit_rate, decay, value, key = [vec_ref[i] for i in range(5)]
    writes = []
    for q in range(seqs):
        copies[q].wait()
        for h in range(heads):
            b = h * seqs + q
            state = buf[q, h]
            removed = jnp.sum(state * unit[b : b + 1], axis=1, keepdims=True)
            column = jnp.sum(jnp.where(eye, value[b : b + 1], 0.0), axis=1, keepdims=True)
            fresh[q, h] = (
                state * decay[b : b + 1]
                - removed * unit_rate[b : b + 1]
                + column * key[b : b + 1]
            )
        write = pltpu.make_async_copy(fresh.at[q], out_ref.at[layer, q], out_sems.at[q])
        write.start()
        writes.append(write)
    for write in writes:
        write.wait()


def update(layer, vecs, states, previous):
    block = states.shape[1:]
    extra = [] if previous is None else [previous]
    return pl.pallas_call(
        functools.partial(update_kernel, layer),
        in_specs=[VMEM, HBM] + [HBM] * len(extra),
        out_specs=HBM,
        out_shape=jax.ShapeDtypeStruct(states.shape, states.dtype),
        input_output_aliases={2: 0} if extra else {},
        scratch_shapes=[
            pltpu.VMEM(block, jnp.float32),
            pltpu.VMEM(block, jnp.float32),
            pltpu.SemaphoreType.DMA((block[0],)),
            pltpu.SemaphoreType.DMA((block[0],)),
        ],
        compiler_params=pltpu.CompilerParams(vmem_limit_bytes=16 << 20),
        cost_estimate=pl.CostEstimate(flops=10**6, bytes_accessed=4 << 20, transcendentals=0),
        name=f"update{layer}",
    )(vecs, states, *extra)


def out_kernel(layer, me_ref, *refs):
    weight_ref, own_ref, sent_ref = refs[-3:]
    parts = refs[:-3]
    rows = parts[0].shape[0]
    mixed = jnp.concatenate([f32(ref[...]) for ref in parts], axis=0).astype(jnp.bfloat16)
    part = jnp.dot(mixed, weight_ref[layer], preferred_element_type=jnp.float32)
    part = swap_blocks(part, me_ref[0], rows, len(parts))
    own_ref[...] = part
    sent_ref[...] = part.astype(jnp.bfloat16)


def out_project(layer, me, parts, weight):
    shape = (len(parts) * parts[0].shape[0], weight.shape[2])
    return pl.pallas_call(
        functools.partial(out_kernel, layer),
        in_specs=[SMEM] + [VMEM] * (len(parts) + 1),
        out_specs=[VMEM, VMEM],
        out_shape=[
            jax.ShapeDtypeStruct(shape, jnp.float32),
            jax.ShapeDtypeStruct(shape, jnp.bfloat16),
        ],
        compiler_params=pltpu.CompilerParams(vmem_limit_bytes=16 << 20),
        name=f"out{layer}",
    )(me, *parts, weight)


def swap(x, axis, n, s):
    return lax.ppermute(x, axis, [(i, i ^ s) for i in range(n)])


def send_order(n, near_first):
    steps = list(range(1, n))
    return steps if near_first else steps[::-1]


def per_device(n_dp, n_tp, stream, states, norm_gain, *rest):
    weights = rest[:ROLES]
    out_weight, decay_bias, head_gain = rest[ROLES:]
    me = lax.axis_index("dp").astype(jnp.int32).reshape(1)
    features = stream.shape[1] * n_dp
    current = stream
    branches = []
    fresh = None
    for layer in range(states.shape[0]):
        (own, *sent), current = project(
            layer, me, current, branches, norm_gain, weights, n_dp, fresh
        )
        got = [swap(sent[s - 1], "dp", n_dp, s) for s in send_order(n_dp, False)]
        mixed, vecs = mix(layer, features, own, got, decay_bias, head_gain, states)
        pieces = {s: swap(mixed, "dp", n_dp, s) for s in send_order(n_dp, True)}
        pieces = [mixed] + [pieces[s] for s in range(1, n_dp)]
        fresh = update(layer, vecs, states, fresh)
        part, part_sent = out_project(layer, me, pieces, out_weight)
        branches = [part] + [swap(part_sent, "tp", n_tp, s) for s in send_order(n_tp, True)]
    total = branches[0]
    for x in branches[1:]:
        total = total + f32(x)
    return (f32(current) + total).astype(jnp.bfloat16), fresh


def solution(mesh):
    in_specs = (
        P("grp", "dp"),
        P(None, ("grp", "dp"), "tp", None, None),
        P(None, "dp"),
        P(None, "dp", "tp"),
        P(None, "dp", "tp"),
        P(None, "dp", "tp"),
        P(None, "dp", "tp"),
        P(None, "dp", "tp"),
        P(None, "dp", "tp"),
        P(None, "tp", "dp"),
        P(None, "tp"),
        P(None, "tp"),
    )
    out_specs = (P("grp", "dp"), P(None, ("grp", "dp"), "tp", None, None))
    return jax.shard_map(
        functools.partial(per_device, mesh.shape["dp"], mesh.shape["tp"]),
        mesh=mesh,
        in_specs=in_specs,
        out_specs=out_specs,
        check_vma=False,
    )
```
